128 devices in a mesh: sp: 16 (over z, x), tp: 8 (over y, core).
Axes of the slice: x: 4, y: 4, z: 4, core: 2. Of those that a mesh axis runs over, the one named last changes fastest.
Arguments:
- stream: bfloat16 [4096, 2048], P(('sp', 'tp')), may hold values from -5 to 5
- out_gate: bfloat16 [4096, 2048], P('sp', 'tp'), may hold values from -6 to 6
- in_gate: bfloat16 [4096, 2048], P('sp', 'tp'), may hold values from -6 to 6
- values: bfloat16 [4096, 2048], P('sp', 'tp'), may hold values from -6 to 6
- conv_weight: float32 [3, 2048], P(None, 'tp'), may hold values from -3 to 3
- out_weight: bfloat16 [2048, 2048], replicated, may hold values from -0.125 to 0.125
- doc_ids: int32 [4096], P('sp'), may hold values from 0 to 5, never falling along the last dimension, each value on 1 to 1024 neighbouring positions
- routes: int32 [4096, 2], P(('sp', 'tp')), may hold values from 0 to 15, all different within a row; in each aligned block of 32 rows (0 to 31, 32 to 63, ...) at most 5 rows name the same one
- route_weight: float32 [4096, 2], P(('sp', 'tp')), may hold values from 0.2 to 1
- norm_gain: float32 [2, 2048], replicated, may hold values from 0.1 to 1.9
- norm_bias: float32 [2, 2048], replicated, may hold values from -2 to 2
- expert_gate: bfloat16 [16, 2048, 7168], P('sp', None, 'tp'), may hold values from -0.125 to 0.125
- expert_up: bfloat16 [16, 2048, 7168], P('sp', None, 'tp'), may hold values from -0.125 to 0.125
- expert_down: bfloat16 [16, 7168, 2048], P('sp', 'tp'), may hold values from -0.0625 to 0.0625
Outputs:
- layer_out: bfloat16 [4096, 2048], P(('sp', 'tp'))
The draws below stay inside these ranges and needn't reach their ends.
Inputs may be any that keep to these rules, and one draw needn't show every extreme that they name: `doc_ids`: each document occupies consecutive positions, numbers never fall along positions, each document has at most 1024 positions and one has exactly 1024. `routes`: each row names two different experts. In each aligned block of 32 rows (the rows of one device) no expert is named more than 5 times, a bound that some block reaches.
All inputs are finite; a program needn't handle non-finite values.
Results may differ from the reference program's by a relative error of at most 0.012.
Values may be sent and summed in bfloat16 or wider, within the bound.
No kernel may reach another device: no remote copies, remote signals or barrier semaphores. Data moves between devices by JAX's collectives and lax.ppermute only.
A program may use at most 64 MiB of HBM per device.

```python
import math
import jax
import jax.numpy as jnp
import numpy as np
from jax import lax

D = 2048
FF = 7168
TOK_DEV = 256
TOKENS = 4096
EXPERTS = 16
CAP = 5
DOCS = 6
DOC_MOST = 1024
N_SP = 16
N_TP = 8


def levels(rng, dims, cuts, smallest, largest):
    def one(position, blocks):
        heights = jax.random.uniform(jax.random.fold_in(jax.random.fold_in(rng, 6), position), (blocks,), jnp.float32, smallest / len(cuts), largest / len(cuts))
        return jnp.repeat(jnp.exp(heights), dims[position] // blocks).reshape((-1,) + (1,) * (len(dims) - position - 1))

    level = one(*cuts[0])
    for cut in cuts[1:]:
        level = level * one(*cut)
    return level


def profile(number_of, total, limit, lean):
    portions = [(1 << 20) // math.isqrt(standing ** lean) + 1 for standing in range(2, number_of + 1)]
    rest, counts = total - limit - (number_of - 1), [1] * (number_of - 1)
    while rest > 0:
        candidates = [i for i in range(number_of - 1) if counts[i] < limit]
        mass, budget = sum([portions[i] for i in candidates]), rest
        for i in candidates:
            addition = min(limit - counts[i], max(1, budget * portions[i] // mass), rest)
            counts[i] = counts[i] + addition
            rest = rest - addition
    return np.array([limit] + counts)


def ragged(stream_key, amount, total, limit, slope):
    if amount == 2:
        one = jax.random.randint(stream_key, (), max(1, total - limit), min(limit, total - 1) + 1)
        return jnp.stack([one, total - one])
    sizes = jnp.asarray(profile(amount, total, limit, slope), jnp.int32)
    couples = (amount - 1) // 2
    donor, receiver = sizes[1:1 + 2 * couples:2], sizes[2:2 + 2 * couples:2]
    margin = jnp.minimum(donor - 1, limit - receiver)
    passed = jax.random.randint(jax.random.fold_in(stream_key, 1), (couples,), 0, 1 << 20) % (margin + 1)
    sizes = sizes.at[1:1 + 2 * couples:2].set(donor - passed).at[2:2 + 2 * couples:2].set(receiver + passed)
    return sizes[jax.random.permutation(jax.random.fold_in(stream_key, 2), amount)]


def routed_block(rng, own, number, rows, number_of, top, bound, lean):
    ranking = jax.random.permutation(rng, number_of)
    crowded, usual = shares(number_of, rows * top, bound, lean, True), shares(number_of, rows * top, bound, lean, False)
    places = jnp.arange(number_of)

    def named(sizes, turn):
        used = int((sizes > 0).sum())
        fixed = max(1, used // 4)
        shifted = fixed + (places - fixed + turn * (used - fixed)) % max(1, number_of - fixed)
        return jnp.zeros((number_of,), jnp.int32).at[ranking[jnp.where(places < fixed, places, shifted)]].set(jnp.asarray(sizes, jnp.int32))

    sizes = jnp.where(number % 4 == 0, named(crowded, number // 4), named(usual, number - number // 4 - 1))
    mixed = jax.random.permutation(jax.random.fold_in(own, 3), number_of)
    giver, sink = mixed[0:number_of // 2 * 2:2], mixed[1:number_of // 2 * 2:2]
    margin = jnp.minimum(sizes[giver] - 1, bound - sizes[sink]) // 2
    margin = jnp.where((giver == ranking[0]) | (sink == ranking[0]) | (sizes[sink] == 0), 0, jnp.maximum(margin, 0))
    shifted = jax.random.randint(jax.random.fold_in(own, 4), (number_of // 2,), 0, 1 << 20) % (margin + 1)
    sizes = sizes.at[giver].add(-shifted).at[sink].add(shifted)
    items = jnp.searchsorted(jnp.cumsum(sizes), jnp.arange(rows * top), side="right").astype(jnp.int32)
    listing = items.reshape(top, rows).T
    listing = listing[jax.random.permutation(jax.random.fold_in(own, 1), rows)]
    turn = jax.random.randint(jax.random.fold_in(own, 2), (rows, 1), 0, top)
    return jnp.take_along_axis(listing, (jnp.arange(top)[None, :] + turn) % top, axis=1)


def shares(amount, total, bound, skew, full):
    portions = [(1 << 20) // math.isqrt(standing ** skew) + 1 for standing in range(1, amount + 1)]
    largest = bound if full else min(bound, max(-(-total // amount), total * portions[0] // sum(portions)))
    least = 1 if total - largest >= amount - 1 else 0
    holding, spare = [largest] + [least] * (amount - 1), total - largest - least * (amount - 1)
    while spare > 0:
        candidates = [i for i in range(1, amount) if holding[i] < largest] or [i for i in range(1, amount) if holding[i] < bound]
        mass, left = sum([portions[i] for i in candidates]), spare
        for i in candidates:
            extra = min(bound - holding[i], max(1, left * portions[i] // mass), spare)
            holding[i] = holding[i] + extra
            spare = spare - extra
    return np.array(holding)


def noise(rng, extent, scale, bound, pieces=(), kind=jnp.bfloat16):
    values = jax.random.normal(rng, extent, jnp.float32) * scale
    if len(pieces) > 0:
        values = levels(rng, extent, pieces, -0.22, 0.18) * values
    return jnp.clip(values, min=-bound, max=bound).astype(kind)


def setup_inputs(seed: int = 0) -> dict:
    key_of = jax.random.split(jax.random.key(seed), 15)
    stream = noise(key_of[0], (TOKENS, D), 0.6, 5.0, ((0, 128),))
    out_gate = noise(key_of[1], (TOKENS, D), 1.0, 6.0, ((0, 16), (1, 8)))
    in_gate = noise(key_of[2], (TOKENS, D), 1.0, 6.0, ((0, 16), (1, 8)))
    values = noise(key_of[3], (TOKENS, D), 1.0, 6.0, ((0, 16), (1, 8)))
    conv_weight = noise(key_of[4], (3, D), 0.577, 3.0, ((1, 8),), jnp.float32)
    out_weight = noise(key_of[5], (D, D), D ** -0.5, 0.125)
    doc_ids = jnp.searchsorted(jnp.cumsum(ragged(key_of[6], DOCS, TOKENS, DOC_MOST, 1)), jnp.arange(TOKENS), side="right").astype(jnp.int32)
    routes_keys = jax.random.split(jax.random.fold_in(key_of[7], 1), TOKENS // (TOK_DEV // N_TP))
    routes_turns = jax.random.permutation(jax.random.fold_in(key_of[7], 3), TOKENS // (TOK_DEV // N_TP))
    routes = jax.vmap(lambda own, number: routed_block(jax.random.fold_in(key_of[7], 2), own, number, TOK_DEV // N_TP, EXPERTS, 2, CAP, 1))(routes_keys, routes_turns).reshape((TOKENS, 2))
    route_weight = jnp.clip(0.2 + 0.8 * jax.random.uniform(key_of[8], (TOKENS, 2), jnp.float32) ** levels(key_of[8], (TOKENS, 2), ((0, 128),), -0.2, 0.2), 0.2, 1.0)
    norm_gain = jnp.clip(1.0 + 0.18 * jax.random.normal(key_of[9], (2, D), jnp.float32), 0.1, 1.9)
    norm_bias = noise(key_of[10], (2, D), 0.3, 2.0, (), jnp.float32)
    expert_gate = noise(key_of[11], (EXPERTS, D, FF), D ** -0.5, 0.125, ((0, 16), (2, 8)))
    expert_up = noise(key_of[12], (EXPERTS, D, FF), D ** -0.5, 0.125, ((0, 16), (2, 8)))
    expert_down = noise(key_of[13], (EXPERTS, FF, D), FF ** -0.5, 0.0625, ((0, 16), (1, 8)))
    return {"stream": stream, "out_gate": out_gate, "in_gate": in_gate, "values": values, "conv_weight": conv_weight, "out_weight": out_weight, "doc_ids": doc_ids, "routes": routes, "route_weight": route_weight, "norm_gain": norm_gain, "norm_bias": norm_bias, "expert_gate": expert_gate, "expert_up": expert_up, "expert_down": expert_down}


residual_scale = 1.6817928

def layer_norm(values_in, gain_row, bias_row):
    row_mean = lax.optimization_barrier(jnp.mean(values_in, axis=-1, keepdims=True))
    centered = values_in - row_mean
    variance = lax.optimization_barrier(jnp.mean(centered * centered, axis=-1, keepdims=True))
    return centered * lax.rsqrt(variance + 1e-05) * gain_row + bias_row

def reference(stream, out_gate, in_gate, values, conv_weight, out_weight, doc_ids, routes, route_weight, norm_gain, norm_bias, expert_gate, expert_up, expert_down):
    length = doc_ids.shape[0]
    gated_values = in_gate.astype(jnp.float32) * values.astype(jnp.float32)
    extended = jnp.pad(gated_values, ((2, 0), (0, 0)))
    ext_docs = jnp.concatenate([jnp.full((2,), -1, jnp.int32), doc_ids])
    keep_first = (ext_docs[1:length + 1] == doc_ids).astype(jnp.float32)[:, None]
    keep_second = (ext_docs[0:length] == doc_ids).astype(jnp.float32)[:, None]
    convolved = conv_weight[0] * extended[0:length] * keep_second + conv_weight[1] * extended[1:length + 1] * keep_first + conv_weight[2] * gated_values
    mixed_rows = (out_gate.astype(jnp.float32) * convolved).astype(jnp.bfloat16)
    projected = jnp.dot(mixed_rows, out_weight, preferred_element_type=jnp.float32)
    normed = layer_norm(residual_scale * stream.astype(jnp.float32) + projected, norm_gain[0], norm_bias[0]).astype(jnp.bfloat16)
    block_rows = TOK_DEV // N_TP
    sources = N_SP * N_TP
    expert_ids = routes.reshape(sources, 2 * block_rows)
    onehot = (expert_ids[:, :, None] == jnp.arange(EXPERTS, dtype=jnp.int32)[None, None, :]).astype(jnp.int32)
    slot_rank = lax.optimization_barrier(jnp.sum((jnp.cumsum(onehot, axis=1) - onehot) * onehot, axis=-1)).astype(jnp.int32)
    source_ids = jnp.arange(sources, dtype=jnp.int32)[:, None]
    dest_rows = (source_ids * CAP + slot_rank).reshape(-1).astype(jnp.int32)
    expert_flat = expert_ids.reshape(-1).astype(jnp.int32)
    repeated = jnp.repeat(normed, 2, axis=0)
    buffer = jnp.zeros((EXPERTS, sources * CAP, D), jnp.bfloat16).at[expert_flat, dest_rows].set(repeated)
    part_width = FF // N_TP

    def expert(expert_item):
        rows, gate_w, up_w, down_w = expert_item
        gate_part = jnp.dot(rows, gate_w, preferred_element_type=jnp.float32)
        up_part = jnp.dot(rows, up_w, preferred_element_type=jnp.float32)
        hidden = (jax.nn.silu(gate_part) * up_part).astype(jnp.bfloat16)
        accumulated = jnp.zeros((rows.shape[0], D), jnp.float32)
        for shard in range(N_TP):
            partial_value = jnp.dot(hidden[:, shard * part_width:(shard + 1) * part_width], down_w[shard * part_width:(shard + 1) * part_width], preferred_element_type=jnp.float32).astype(jnp.bfloat16)
            partial_value = lax.optimization_barrier(partial_value)
            accumulated = accumulated + partial_value.astype(jnp.float32)
        return accumulated.astype(jnp.bfloat16)
    outputs = lax.map(expert, (buffer, expert_gate, expert_up, expert_down))
    picked = outputs[expert_flat, dest_rows].astype(jnp.float32).reshape(length, 2, D)
    routed_sum = lax.optimization_barrier(jnp.sum(picked * route_weight[:, :, None], axis=1))
    return layer_norm(residual_scale * normed.astype(jnp.float32) + routed_sum, norm_gain[1], norm_bias[1]).astype(jnp.bfloat16)
```

```python
import jax
import jax.numpy as jnp
from jax import lax
from jax.experimental import pallas as pl
from jax.experimental.pallas import tpu as pltpu
from jax.sharding import Mesh
from jax.sharding import PartitionSpec as P


RES = 1.6817928
F32 = jnp.float32
BF16 = jnp.bfloat16
MIB = 1 << 20
SLOTS = 5
LANES = 128


def call(kernel, outs, *args, scratch=(), limit=16, flops=0, name=None):
    moved = sum(a.size * a.dtype.itemsize for a in (*args, *outs))
    return pl.pallas_call(
        kernel,
        out_shape=outs,
        in_specs=[pl.BlockSpec(memory_space=pltpu.VMEM)] * len(args),
        out_specs=[pl.BlockSpec(memory_space=pltpu.VMEM)] * len(outs),
        scratch_shapes=scratch,
        compiler_params=pltpu.CompilerParams(vmem_limit_bytes=limit * MIB),
        cost_estimate=pl.CostEstimate(flops=flops, bytes_accessed=moved, transcendentals=0),
        name=name,
    )(*args)


def sds(shape, dtype):
    return jax.ShapeDtypeStruct(shape, dtype)


def column(row):
    n = row.shape[1]
    eye = lax.broadcasted_iota(jnp.int32, (n, n), 0) == lax.broadcasted_iota(jnp.int32, (n, n), 1)
    return jnp.sum(jnp.where(eye, jnp.broadcast_to(row, (n, n)), 0.0), axis=1, keepdims=True)


def layer_norm(v, gain, bias):
    mean = jnp.mean(v, axis=-1, keepdims=True)
    centered = v - mean
    var = jnp.mean(centered * centered, axis=-1, keepdims=True)
    return centered * lax.rsqrt(var + 1e-5) * gain + bias


def slots_of(routes_ref, experts):
    rows = routes_ref.shape[1]
    names = lax.broadcasted_iota(jnp.int32, (experts, rows), 0)
    hot = [(names == routes_ref[k : k + 1, :]).astype(F32) for k in range(2)]
    earlier = lax.broadcasted_iota(jnp.int32, (rows, rows), 0) < lax.broadcasted_iota(
        jnp.int32, (rows, rows), 1
    )
    before = jnp.dot(
        (hot[0] + hot[1]).astype(BF16), earlier.astype(F32).astype(BF16), preferred_element_type=F32
    )
    return [
        jnp.sum(before * h, axis=0, keepdims=True)
        + routes_ref[k : k + 1, :].astype(F32) * float(SLOTS)
        for k, h in enumerate(hot)
    ]


def conv_kernel(in_gate, values, out_gate, weight, docs, halo, out, gs, ds):
    n = in_gate.shape[0]
    gated = in_gate[...].astype(F32) * values[...].astype(F32)
    gs[8 : 8 + n, :] = gated
    gs[6:8, :] = halo[0:2, :].astype(F32) * halo[2:4, :].astype(F32)
    doc = jnp.broadcast_to(column(docs[...].astype(F32)), (n, LANES))
    ds[8 : 8 + n, :] = doc
    ds[6:8, :] = halo[4:6, 0:LANES].astype(F32)
    keep1 = ds[7 : 7 + n, :] == doc
    keep2 = ds[6 : 6 + n, :] == doc
    for j in range(in_gate.shape[1] // LANES):
        at = slice(j * LANES, (j + 1) * LANES)
        mixed = (
            weight[0:1, at] * jnp.where(keep2, gs[6 : 6 + n, at], 0.0)
            + weight[1:2, at] * jnp.where(keep1, gs[7 : 7 + n, at], 0.0)
            + weight[2:3, at] * gs[8 : 8 + n, at]
        )
        out[:, at] = (out_gate[:, at].astype(F32) * mixed).astype(BF16)


def store_packed(rows, packed, tmp):
    n, d = rows.shape
    pieces = d // LANES
    for k in range(pieces):
        tmp[pl.ds(k, n, stride=pieces), :] = rows[:, k * LANES : (k + 1) * LANES]
    packed[...] = tmp[...].astype(packed.dtype)


def load_packed(packed, out, tmp):
    n, d = out.shape
    pieces = d // LANES
    tmp[...] = packed[...].astype(F32)
    for k in range(pieces):
        out[:, k * LANES : (k + 1) * LANES] = tmp[pl.ds(k, n, stride=pieces), :].astype(out.dtype)


def project_kernel(experts, tokens, out_weight, stream, gain, bias, routes, normed_out, send, tmp):
    parts, rows, width = tokens.shape
    total = RES * stream[...].astype(F32)
    for j in range(parts):
        total += jnp.dot(
            tokens[j], out_weight[j * width : (j + 1) * width, :], preferred_element_type=F32
        )
    normed = layer_norm(total, gain[0:1, :], bias[0:1, :]).astype(BF16)
    normed_out[...] = normed
    slots = slots_of(routes, experts)
    place = lax.broadcasted_iota(jnp.int32, (experts * SLOTS, rows), 0).astype(F32)
    chosen = (place == slots[0]) | (place == slots[1])
    sent = jnp.dot(chosen.astype(F32).astype(BF16), normed, preferred_element_type=F32)
    store_packed(sent, send, tmp)


def unpack_kernel(packed, out, tmp):
    load_packed(packed, out, tmp)


def expert_kernel(mine, other, gate, up, down, keep, give, rows, hidden):
    n = mine.shape[0]
    rows[0:n, :] = mine[...]
    rows[n : 2 * n, :] = other[...]
    x = rows[...]
    g = jnp.dot(x, gate[...], preferred_element_type=F32)
    u = jnp.dot(x, up[...], preferred_element_type=F32)
    hidden[...] = (g / (1.0 + jnp.exp(-g)) * u).astype(BF16)
    part = jnp.dot(hidden[...], down[...], preferred_element_type=F32).astype(BF16)
    keep[...] = part[0:n, :]
    give[...] = part[n : 2 * n, :]


def pack_sum_kernel(a, b, c, d, out, tmp):
    total = (a[...].astype(F32) + b[...].astype(F32)) + (c[...].astype(F32) + d[...].astype(F32))
    store_packed(total, out, tmp)


def combine_kernel(experts, packed, routes, route_weight, normed, gain, bias, out, tmp, got):
    rows = normed.shape[0]
    load_packed(packed, got, tmp)
    slots = slots_of(routes, experts)
    place = lax.broadcasted_iota(jnp.int32, (rows, experts * SLOTS), 1).astype(F32)
    total = RES * normed[...].astype(F32)
    for k in range(2):
        pick = (place == column(slots[k])).astype(F32).astype(BF16)
        total += column(route_weight[k : k + 1, :]) * jnp.dot(
            pick, got[...], preferred_element_type=F32
        )
    out[...] = layer_norm(total, gain[1:2, :], bias[1:2, :]).astype(BF16)


def shifted(value, axis, steps):
    count = lax.axis_size(axis)
    return lax.ppermute(value, axis, [(i, (i + steps) % count) for i in range(count)])


def swapped(value):
    return lax.ppermute(value, "c", [(0, 1), (1, 0)])


def shards(
    stream,
    out_gate,
    in_gate,
    values,
    conv_weight,
    out_weight,
    doc_ids,
    routes,
    route_weight,
    norm_gain,
    norm_bias,
    expert_gate,
    expert_up,
    expert_down,
):
    length, width = in_gate.shape
    rows, model = stream.shape
    experts = lax.axis_size("sp")
    chips = lax.axis_size("y")
    group = chips * lax.axis_size("c")
    pieces = model // LANES
    tail_docs = jnp.broadcast_to(doc_ids[length - 2 :].astype(BF16)[:, None], (2, width))
    tail = jnp.concatenate(
        [in_gate[length - 2 :], values[length - 2 :], tail_docs, tail_docs], axis=0
    )
    halo = lax.ppermute(tail, "sp", [(i, i + 1) for i in range(experts - 1)])
    (mixed,) = call(
        conv_kernel,
        [sds((length, width), BF16)],
        in_gate,
        values,
        out_gate,
        conv_weight,
        doc_ids[None, :],
        halo,
        scratch=[pltpu.VMEM((length + 8, width), F32), pltpu.VMEM((length + 8, LANES), F32)],
        limit=8,
        name="conv",
    )
    tokens = lax.all_to_all(
        mixed.reshape(group, rows, width), ("y", "c"), split_axis=0, concat_axis=0, tiled=True
    )
    routes_t, weight_t = routes.T, route_weight.T
    flat = experts * SLOTS * pieces
    normed, send = call(
        lambda *refs: project_kernel(experts, *refs),
        [sds((rows, model), BF16), sds((flat, LANES), BF16)],
        tokens,
        out_weight,
        stream,
        norm_gain,
        norm_bias,
        routes_t,
        scratch=[pltpu.VMEM((flat, LANES), F32)],
        limit=16,
        flops=2 * rows * model * model,
        name="project",
    )
    arrived = lax.all_to_all(
        send.reshape(experts, SLOTS * pieces, LANES), "sp", split_axis=0, concat_axis=0, tiled=True
    )
    slots = experts * SLOTS
    (mine,) = call(
        unpack_kernel,
        [sds((slots, model), BF16)],
        arrived.reshape(flat, LANES),
        scratch=[pltpu.VMEM((flat, LANES), F32)],
        limit=8,
        name="unpack",
    )
    order = [0, 1, chips - 1] + list(range(2, chips - 1))
    held = {k: mine if k == 0 else shifted(mine, "y", k) for k in order}
    gate, up, down = expert_gate[0], expert_up[0], expert_down[0]
    hidden_units = gate.shape[1]
    back = []
    for k in order:
        keep, give = call(
            expert_kernel,
            [sds((slots, model), BF16), sds((slots, model), BF16)],
            held[k],
            swapped(held[k]),
            gate,
            up,
            down,
            scratch=[pltpu.VMEM((2 * slots, model), BF16), pltpu.VMEM((2 * slots, hidden_units), BF16)],
            limit=20,
            flops=2 * 2 * slots * 3 * model * hidden_units,
            name="expert",
        )
        pair = (keep.astype(F32) + swapped(give).astype(F32)).astype(BF16)
        back.append(pair if k == 0 else shifted(pair, "y", -k))
    (result,) = call(
        pack_sum_kernel,
        [sds((flat, LANES), BF16)],
        *back,
        scratch=[pltpu.VMEM((flat, LANES), F32)],
        limit=8,
        name="pack_sum",
    )
    returned = lax.all_to_all(
        result.reshape(experts, SLOTS * pieces, LANES), "sp", split_axis=0, concat_axis=0, tiled=True
    )
    (out,) = call(
        lambda *refs: combine_kernel(experts, *refs),
        [sds((rows, model), BF16)],
        returned.reshape(flat, LANES),
        routes_t,
        weight_t,
        normed,
        norm_gain,
        norm_bias,
        scratch=[pltpu.VMEM((flat, LANES), F32), pltpu.VMEM((slots, model), BF16)],
        limit=8,
        name="combine",
    )
    return out


def solution(mesh):
    fine = Mesh(mesh.devices.reshape(mesh.shape["sp"], mesh.shape["tp"] // 2, 2), ("sp", "y", "c"))
    tp = ("y", "c")
    every = ("sp", "y", "c")
    in_specs = (
        P(every, None),
        P("sp", tp),
        P("sp", tp),
        P("sp", tp),
        P(None, tp),
        P(),
        P("sp"),
        P(every, None),
        P(every, None),
        P(),
        P(),
        P("sp", None, tp),
        P("sp", None, tp),
        P("sp", tp, None),
    )
    return jax.shard_map(
        shards, mesh=fine, in_specs=in_specs, out_specs=P(every, None), check_vma=False
    )
```

```python
import jax
import jax.numpy as jnp
from jax import lax
from jax.experimental import pallas as pl
from jax.experimental.pallas import tpu as pltpu
from jax.sharding import Mesh
from jax.sharding import PartitionSpec as P


RES = 1.6817928
F32 = jnp.float32
BF16 = jnp.bfloat16
MIB = 1 << 20
SLOTS = 5
LANES = 128


def call(kernel, outs, *args, scratch=(), limit=16, flops=0, space=pltpu.VMEM):
    if space is pltpu.HBM:
        args = [pltpu.with_memory_space_constraint(a, pltpu.HBM) for a in args]
    moved = sum(a.size * a.dtype.itemsize for a in (*args, *outs))
    return pl.pallas_call(
        kernel,
        out_shape=outs,
        in_specs=[pl.BlockSpec(memory_space=space)] * len(args),
        out_specs=[pl.BlockSpec(memory_space=pltpu.VMEM)] * len(outs),
        scratch_shapes=scratch,
        compiler_params=pltpu.CompilerParams(vmem_limit_bytes=limit * MIB),
        cost_estimate=pl.CostEstimate(flops=flops, bytes_accessed=moved, transcendentals=0),
    )(*args)


def sds(shape, dtype):
    return jax.ShapeDtypeStruct(shape, dtype)


def column(row):
    n = row.shape[1]
    eye = lax.broadcasted_iota(jnp.int32, (n, n), 0) == lax.broadcasted_iota(jnp.int32, (n, n), 1)
    return jnp.sum(jnp.where(eye, jnp.broadcast_to(row, (n, n)), 0.0), axis=1, keepdims=True)


def layer_norm(v, gain, bias):
    mean = jnp.mean(v, axis=-1, keepdims=True)
    centered = v - mean
    var = jnp.mean(centered * centered, axis=-1, keepdims=True)
    return centered * lax.rsqrt(var + 1e-5) * gain + bias


def slots_of(routes_ref, experts):
    rows = routes_ref.shape[1]
    names = lax.broadcasted_iota(jnp.int32, (experts, rows), 0)
    hot = [(names == routes_ref[k : k + 1, :]).astype(F32) for k in range(2)]
    earlier = lax.broadcasted_iota(jnp.int32, (rows, rows), 0) < lax.broadcasted_iota(
        jnp.int32, (rows, rows), 1
    )
    before = jnp.dot(
        (hot[0] + hot[1]).astype(BF16), earlier.astype(F32).astype(BF16), preferred_element_type=F32
    )
    return [
        jnp.sum(before * h, axis=0, keepdims=True)
        + routes_ref[k : k + 1, :].astype(F32) * float(SLOTS)
        for k, h in enumerate(hot)
    ]


def fetch(sources, targets, sems):
    copies = [
        pltpu.make_async_copy(a, b, sems.at[i]) for i, (a, b) in enumerate(zip(sources, targets))
    ]
    for c in copies:
        c.start()
    for c in copies:
        c.wait()


def load_kernel(*refs):
    count = (len(refs) - 1) // 2
    fetch(refs[:count], refs[count : 2 * count], refs[-1])


def loaded(*arrays, limit=1):
    return call(
        load_kernel,
        [sds(a.shape, a.dtype) for a in arrays],
        *arrays,
        scratch=[pltpu.SemaphoreType.DMA((len(arrays),))],
        limit=limit,
        space=pltpu.HBM,
    )


def begin_kernel(*refs):
    count = (len(refs) - 2) // 2
    tail, sems = refs[-2:]
    targets = refs[count : 2 * count]
    fetch(refs[:count], targets, sems)
    in_gate, values, docs = targets[0], targets[1], targets[4]
    n, width = in_gate.shape
    last = docs[0:1, n - LANES : n].astype(F32)
    lane = lax.broadcasted_iota(jnp.int32, (1, LANES), 1)
    tail[0:2, :] = in_gate[n - 2 : n, :]
    tail[2:4, :] = values[n - 2 : n, :]
    for j in range(2):
        doc = jnp.sum(jnp.where(lane == LANES - 2 + j, last, 0.0), axis=1, keepdims=True)
        for row in (4 + j, 6 + j):
            tail[row : row + 1, :] = jnp.broadcast_to(doc, (1, width)).astype(BF16)


def conv_kernel(in_gate, values, out_gate, weight, docs, halo, own, sib, gs, ds, ms):
    n = in_gate.shape[0]
    gated = in_gate[...].astype(F32) * values[...].astype(F32)
    gs[8 : 8 + n, :] = gated
    gs[6:8, :] = halo[0:2, :].astype(F32) * halo[2:4, :].astype(F32)
    doc = jnp.broadcast_to(column(docs[...].astype(F32)), (n, LANES))
    ds[8 : 8 + n, :] = doc
    ds[6:8, :] = halo[4:6, 0:LANES].astype(F32)
    keep1 = ds[7 : 7 + n, :] == doc
    keep2 = ds[6 : 6 + n, :] == doc
    for j in range(in_gate.shape[1] // LANES):
        at = slice(j * LANES, (j + 1) * LANES)
        mixed = (
            weight[0:1, at] * jnp.where(keep2, gs[6 : 6 + n, at], 0.0)
            + weight[1:2, at] * jnp.where(keep1, gs[7 : 7 + n, at], 0.0)
            + weight[2:3, at] * gs[8 : 8 + n, at]
        )
        ms[:, at] = (out_gate[:, at].astype(F32) * mixed).astype(BF16)
    chips, rows = own.shape[:2]
    y, c = lax.axis_index("y"), lax.axis_index("c")
    for k in range(chips):
        to = lax.rem(y + k, chips) * 2
        own[k] = ms[pl.ds(pl.multiple_of((to + c) * rows, rows), rows), :]
        sib[k] = ms[pl.ds(pl.multiple_of((to + 1 - c) * rows, rows), rows), :]


def store_packed(rows, packed, tmp):
    n, d = rows.shape
    pieces = d // LANES
    for k in range(pieces):
        tmp[pl.ds(k, n, stride=pieces), :] = rows[:, k * LANES : (k + 1) * LANES]
    packed[...] = tmp[...].astype(packed.dtype)


def load_packed(packed, out, tmp):
    n, d = out.shape
    pieces = d // LANES
    tmp[...] = packed[...].astype(F32)
    for k in range(pieces):
        out[:, k * LANES : (k + 1) * LANES] = tmp[pl.ds(k, n, stride=pieces), :].astype(out.dtype)


def project_kernel(experts, *refs):
    chips = lax.axis_size("y")
    own, sib = refs[0:2]
    came = refs[2 : 1 + chips]
    out_weight, stream, gain, bias, routes, normed_out, send, tmp = refs[1 + chips :]
    rows, width = own.shape[1:]
    y, c = lax.axis_index("y"), lax.axis_index("c")
    total = RES * stream[...].astype(F32)
    for k in range(chips):
        source = lax.rem(y - k + chips, chips) * 2
        for j, channels in enumerate((source + c, source + 1 - c)):
            part = (own, sib)[j][0] if k == 0 else came[k - 1][j]
            at = pl.ds(pl.multiple_of(channels * width, width), width)
            total += jnp.dot(part, out_weight[at, :], preferred_element_type=F32)
    normed = layer_norm(total, gain[0:1, :], bias[0:1, :]).astype(BF16)
    normed_out[...] = normed
    slots = slots_of(routes, experts)
    place = lax.broadcasted_iota(jnp.int32, (experts * SLOTS, rows), 0).astype(F32)
    chosen = (place == slots[0]) | (place == slots[1])
    sent = jnp.dot(chosen.astype(F32).astype(BF16), normed, preferred_element_type=F32)
    store_packed(sent, send, tmp)


def unpack_kernel(packed, out, tmp):
    load_packed(packed, out, tmp)


def expert_kernel(mine, other, gate, up, down, keep, give, rows, hidden):
    n = mine.shape[0]
    rows[0:n, :] = mine[...]
    rows[n : 2 * n, :] = other[...]
    x = rows[...]
    g = jnp.dot(x, gate[...], preferred_element_type=F32)
    u = jnp.dot(x, up[...], preferred_element_type=F32)
    hidden[...] = (g / (1.0 + jnp.exp(-g)) * u).astype(BF16)
    part = jnp.dot(hidden[...], down[...], preferred_element_type=F32).astype(BF16)
    keep[...] = part[0:n, :]
    give[...] = part[n : 2 * n, :]


def pack_sum_kernel(a, b, c, d, out, tmp):
    total = (a[...].astype(F32) + b[...].astype(F32)) + (c[...].astype(F32) + d[...].astype(F32))
    store_packed(total, out, tmp)


def combine_kernel(experts, packed, routes, route_weight, normed, gain, bias, out, tmp, got):
    rows = normed.shape[0]
    load_packed(packed, got, tmp)
    slots = slots_of(routes, experts)
    place = lax.broadcasted_iota(jnp.int32, (rows, experts * SLOTS), 1).astype(F32)
    total = RES * normed[...].astype(F32)
    for k in range(2):
        pick = (place == column(slots[k])).astype(F32).astype(BF16)
        total += column(route_weight[k : k + 1, :]) * jnp.dot(
            pick, got[...], preferred_element_type=F32
        )
    out[...] = layer_norm(total, gain[1:2, :], bias[1:2, :]).astype(BF16)


def shifted(value, axis, steps):
    count = lax.axis_size(axis)
    return lax.ppermute(value, axis, [(i, (i + steps) % count) for i in range(count)])


def swapped(value):
    return lax.ppermute(value, "c", [(0, 1), (1, 0)])


def shards(
    stream,
    out_gate,
    in_gate,
    values,
    conv_weight,
    out_weight,
    doc_ids,
    routes,
    route_weight,
    norm_gain,
    norm_bias,
    expert_gate,
    expert_up,
    expert_down,
):
    length, width = in_gate.shape
    rows, model = stream.shape
    experts = lax.axis_size("sp")
    chips = lax.axis_size("y")
    pieces = model // LANES
    gates = (in_gate, values, out_gate, conv_weight, doc_ids[None, :])
    *gates, tail = call(
        begin_kernel,
        [*(sds(a.shape, a.dtype) for a in gates), sds((8, width), BF16)],
        *gates,
        scratch=[pltpu.SemaphoreType.DMA((len(gates),))],
        limit=1,
        flops=FLOPS["begin"],
        space=pltpu.HBM,
    )
    halo = lax.ppermute(tail, "sp", [(i, i + 1) for i in range(experts - 1)])
    own, sib = call(
        conv_kernel,
        [sds((chips, rows, width), BF16)] * 2,
        *gates,
        halo,
        scratch=[
            pltpu.VMEM((length + 8, width), F32),
            pltpu.VMEM((length + 8, LANES), F32),
            pltpu.VMEM((length, width), BF16),
        ],
        limit=8,
        flops=FLOPS["conv"],
    )
    sib = swapped(sib)
    came = []
    for k in range(1, chips):
        came.append(shifted(jnp.stack([own[k], sib[k]]), "y", k))
    stream, gain, bias, routes_t, weight_t = loaded(
        stream, norm_gain, norm_bias, routes.T, route_weight.T
    )
    flat = experts * SLOTS * pieces
    normed, send = call(
        lambda *refs: project_kernel(experts, *refs),
        [sds((rows, model), BF16), sds((flat, LANES), BF16)],
        own,
        sib,
        *came,
        out_weight,
        stream,
        gain,
        bias,
        routes_t,
        scratch=[pltpu.VMEM((flat, LANES), F32)],
        limit=4,
        flops=FLOPS["project"],
    )
    arrived = lax.all_to_all(
        send.reshape(experts, SLOTS * pieces, LANES), "sp", split_axis=0, concat_axis=0, tiled=True
    )
    slots = experts * SLOTS
    (mine,) = call(
        unpack_kernel,
        [sds((slots, model), BF16)],
        arrived.reshape(flat, LANES),
        scratch=[pltpu.VMEM((flat, LANES), F32)],
        limit=4,
        flops=FLOPS["unpack"],
    )
    order = ORDER
    held = {0: mine}
    for k in order[1:]:
        held[k] = shifted(mine, "y", k)
    gate, up, down = expert_gate[0], expert_up[0], expert_down[0]
    hidden_units = gate.shape[1]
    back = []
    for k in order:
        other = swapped(held[k])
        keep, give = call(
            expert_kernel,
            [sds((slots, model), BF16), sds((slots, model), BF16)],
            held[k],
            other,
            gate,
            up,
            down,
            scratch=[
                pltpu.VMEM((2 * slots, model), BF16),
                pltpu.VMEM((2 * slots, hidden_units), BF16),
            ],
            limit=12,
            flops=2 * 2 * slots * 3 * model * hidden_units,
        )
        given = swapped(give)
        pair = (keep.astype(F32) + given.astype(F32)).astype(BF16)
        if k:
            pair = shifted(pair, "y", -k)
        back.append(pair)
    (result,) = call(
        pack_sum_kernel,
        [sds((flat, LANES), BF16)],
        *back,
        scratch=[pltpu.VMEM((flat, LANES), F32)],
        limit=4,
    )
    returned = lax.all_to_all(
        result.reshape(experts, SLOTS * pieces, LANES), "sp", split_axis=0, concat_axis=0, tiled=True
    )
    (out,) = call(
        lambda *refs: combine_kernel(experts, *refs),
        [sds((rows, model), BF16)],
        returned.reshape(flat, LANES),
        routes_t,
        weight_t,
        normed,
        gain,
        bias,
        scratch=[pltpu.VMEM((flat, LANES), F32), pltpu.VMEM((slots, model), BF16)],
        limit=4,
    )
    return out


FLOPS = {"begin": 4_000_000_000, "conv": 4_000_000_000, "project": 4_000_000_000, "unpack": 4_000_000_000}
ORDER = (0, 2, 1, 3)


def solution(mesh):
    fine = Mesh(mesh.devices.reshape(mesh.shape["sp"], mesh.shape["tp"] // 2, 2), ("sp", "y", "c"))
    tp = ("y", "c")
    every = ("sp", "y", "c")
    in_specs = (
        P(every, None),
        P("sp", tp),
        P("sp", tp),
        P("sp", tp),
        P(None, tp),
        P(),
        P("sp"),
        P(every, None),
        P(every, None),
        P(),
        P(),
        P("sp", None, tp),
        P("sp", None, tp),
        P("sp", tp, None),
    )
    return jax.shard_map(
        shards, mesh=fine, in_specs=in_specs, out_specs=P(every, None), check_vma=False
    )
```
